1024 devices in a mesh: sp: 64 (over z, core), tp: 16 (over y, x).
Axes of the slice: x: 4, y: 4, z: 32, core: 2. Of those that a mesh axis runs over, the one named last changes fastest.
Arguments:
- tokens: bfloat16 [16384, 4096], P('sp'), may hold values from -6 to 6
- norm_gain: float32 [2, 4096], replicated, may hold values from 0.1 to 1.9
- w_outer: bfloat16 [2, 4096, 1024], P(None, 'sp', 'tp'), may hold values from -0.09375 to 0.09375
- w_inner: bfloat16 [2, 4096, 1024], P(None, 'sp', 'tp'), may hold values from -0.09375 to 0.09375
- w_value: bfloat16 [2, 4096, 1024], P(None, 'sp', 'tp'), may hold values from -0.09375 to 0.09375
- w_back: bfloat16 [2, 1024, 4096], P(None, 'sp', 'tp'), may hold values from -0.1875 to 0.1875
- taps: float32 [2, 3, 1024], P(None, None, 'tp'), may hold values from -3 to 3
Outputs:
- result: bfloat16 [16384, 4096], P('sp', 'tp')
The draws below stay inside these ranges and needn't reach their ends.
All inputs are finite; a program needn't handle non-finite values.
Results may differ from the reference program's by a relative error of at most 0.022.
Values may be sent and summed in bfloat16 or wider, within the bound.
No kernel may reach another device: no remote copies, remote signals or barrier semaphores. Data moves between devices by JAX's collectives and lax.ppermute only.
A program may use at most 32 MiB of HBM per device.

```python
import jax
import jax.numpy as jnp
from jax import lax

D = 4096
MIX = 1024
LAYERS = 2
TAPS = 3
TOKENS = 16384


def level_of(own_key, shape, cuts, low, top_value):
    factor_of = 1.0
    for dim, blocks in cuts:
        draws = jax.random.uniform(jax.random.fold_in(jax.random.fold_in(own_key, 6), dim), (blocks,), jnp.float32, low / len(cuts), top_value / len(cuts))
        factor_of = factor_of * jnp.repeat(jnp.exp(draws), shape[dim] // blocks).reshape((-1,) + (1,) * (len(shape) - 1 - dim))
    return factor_of


def bell_draw(key, extent, spread, bound, split=(), dtype=jnp.bfloat16):
    loudness = level_of(key, extent, split, -0.22, 0.18) if split else 1.0
    result = jax.random.normal(key, extent, jnp.float32) * spread * loudness
    return jnp.minimum(jnp.maximum(result, -bound), bound).astype(dtype)


def setup_inputs(seed: int = 0) -> dict:
    key_list = jax.random.split(jax.random.key(seed), 8)
    return {
        "tokens": bell_draw(key_list[0], (TOKENS, D), 1.0, 6.0, ((0, 64),)),
        "norm_gain": jnp.clip(1.0 + 0.18 * jax.random.normal(key_list[1], (LAYERS, D), jnp.float32), 0.1, 1.9),
        "w_outer": bell_draw(key_list[2], (LAYERS, D, MIX), D ** -0.5, 0.09375, ((1, 64), (2, 16))),
        "w_inner": bell_draw(key_list[3], (LAYERS, D, MIX), D ** -0.5, 0.09375, ((1, 64), (2, 16))),
        "w_value": bell_draw(key_list[4], (LAYERS, D, MIX), D ** -0.5, 0.09375, ((1, 64), (2, 16))),
        "w_back": bell_draw(key_list[5], (LAYERS, MIX, D), MIX ** -0.5, 0.1875, ((1, 64), (2, 16))),
        "taps": bell_draw(key_list[6], (LAYERS, TAPS, MIX), 0.6, 3.0, ((2, 16),), jnp.float32),
    }


eps = 1e-06

def reference(tokens, norm_gain, w_outer, w_inner, w_value, w_back, taps):
    current = tokens
    for layer in range(LAYERS):
        xf = current.astype(jnp.float32)
        normed = (xf * lax.rsqrt(lax.optimization_barrier(jnp.mean(xf * xf, axis=-1, keepdims=True)) + eps) * norm_gain[layer]).astype(jnp.bfloat16)
        outer = jnp.dot(normed, w_outer[layer], preferred_element_type=jnp.float32).astype(jnp.bfloat16)
        inner = jnp.dot(normed, w_inner[layer], preferred_element_type=jnp.float32).astype(jnp.bfloat16)
        value = jnp.dot(normed, w_value[layer], preferred_element_type=jnp.float32).astype(jnp.bfloat16)
        mixed = (inner.astype(jnp.float32) * value.astype(jnp.float32)).astype(jnp.bfloat16)
        padded = jnp.pad(mixed.astype(jnp.float32), ((2, 0), (0, 0)))
        conv = taps[layer, 0] * padded[:-2] + taps[layer, 1] * padded[1:-1] + taps[layer, 2] * padded[2:]
        gated = (outer.astype(jnp.float32) * conv).astype(jnp.bfloat16)
        proj = jnp.dot(gated, w_back[layer], preferred_element_type=jnp.float32)
        current = (current.astype(jnp.float32) + proj).astype(jnp.bfloat16)
    return current
```

```python
import functools

import jax
import jax.numpy as jnp
from jax import lax
from jax.experimental import pallas as pl
from jax.experimental.pallas import tpu as pltpu
from jax.sharding import PartitionSpec as P

EPS = 1e-06
HALO = 8
ROWS = 64
CLASS = (-4, 0, -12, 12, 4, 8, -8, 16)
OFFSETS = (
    CLASS
    + tuple(o - 1 for o in CLASS)
    + tuple(o + 1 for o in CLASS)
    + tuple(o - 2 for o in CLASS[:4])
    + tuple(o + 2 for o in CLASS[1:5])
)
VMEM = pl.BlockSpec(memory_space=pltpu.VMEM)
SMEM = pl.BlockSpec(memory_space=pltpu.SMEM)
BF16 = jnp.bfloat16
F32 = jnp.float32


def pack_kernel(wo, wi, wv, wb, *outs):
    for layer, out in enumerate(outs):
        back = wb[layer].astype(F32)
        columns = back.shape[1] // 4
        folded = jnp.concatenate(
            [back[:, k * columns : (k + 1) * columns] for k in range(4)], axis=0
        )
        parts = [w[layer].astype(F32) for w in (wo, wi, wv)] + [folded]
        out[...] = jnp.concatenate(parts, axis=1).astype(BF16)


def pack(wo, wi, wv, wb):
    shape = jax.ShapeDtypeStruct((ROWS, 4 * wo.shape[2]), BF16)
    return pl.pallas_call(
        pack_kernel,
        out_shape=[shape] * wo.shape[0],
        in_specs=[VMEM] * 4,
        out_specs=[VMEM] * wo.shape[0],
    )(wo, wi, wv, wb)


def assemble(pos, mine, other, w):
    z, core = pos[0], pos[1]
    for p, off in enumerate(OFFSETS):
        plane = lax.rem(z + (off + 32), 32)
        own = pl.multiple_of(plane * 128 + core * 64, 64)
        far = pl.multiple_of(plane * 128 + (1 - core) * 64, 64)
        w[pl.ds(own, ROWS), :] = mine[p * ROWS : (p + 1) * ROWS, :]
        w[pl.ds(far, ROWS), :] = other[p * ROWS : (p + 1) * ROWS, :]


def back_weights(w, wb):
    whole = w[:, 128:].reshape(64, 4, 16, 128)
    for k in range(4):
        wb[:, k * 128 : (k + 1) * 128] = whole[:, k].reshape(1024, 128)


def rounded(v):
    return v.astype(BF16).astype(F32)


def gate(acc, taps):
    outer, inner, value = (rounded(acc[:, k * 64 : (k + 1) * 64]) for k in range(3))
    mixed = rounded(inner * value)
    rows = mixed.shape[0]
    padded = jnp.concatenate([jnp.zeros((8, 64), F32), mixed], axis=0)
    conv = (
        taps[0:1, :] * padded[6 : 6 + rows]
        + taps[1:2, :] * padded[7 : 7 + rows]
        + taps[2:3, :] * padded[8 : 8 + rows]
    )
    return outer * conv


def store_gated(gated, out, halo):
    half = (gated.shape[0] - HALO) // 2
    main = jnp.concatenate(
        [gated[HALO : HALO + half], gated[HALO + half :]], axis=1
    ).astype(BF16)
    copies = out.shape[0]
    if halo:
        extra = jnp.concatenate([gated[:HALO], gated[:HALO]], axis=1).astype(BF16)
    for j in range(copies):
        out[j, :half, :] = main
        if halo:
            out[j, half:, :] = extra


def first_kernel(pos, x, before, gain, taps, mine, other, out, wb, w):
    assemble(pos, mine, other, w)
    back_weights(w, wb)
    chunks, width = 16, x.shape[1] // 16
    def part(k):
        cols = slice(k * width, (k + 1) * width)
        return jnp.concatenate(
            [before[:, cols].astype(F32), x[:, cols].astype(F32)], axis=0
        )
    squares = None
    for k in range(chunks):
        p = part(k)
        s = jnp.sum(p * p, axis=1, keepdims=True)
        squares = s if squares is None else squares + s
    scale = lax.rsqrt(squares / x.shape[1] + EPS)
    acc = None
    for k in range(chunks):
        cols = slice(k * width, (k + 1) * width)
        normed = (part(k) * scale * gain[0:1, cols]).astype(BF16)
        d = jnp.dot(normed, w[cols, :], preferred_element_type=F32)
        acc = d if acc is None else acc + d
    store_gated(gate(acc, taps[0]), out, True)


def second_kernel(pos, x, gain, taps, mine, other, out, wb, w):
    assemble(pos, mine, other, w)
    back_weights(w, wb)
    chunks, width = x.shape[0], x.shape[2]
    squares = None
    for k in range(chunks):
        p = x[k].astype(F32)
        s = jnp.sum(p * p, axis=1, keepdims=True)
        squares = s if squares is None else squares + s
    scale = lax.rsqrt(squares / (chunks * width) + EPS)
    acc = None
    for k in range(chunks):
        cols = slice(k * width, (k + 1) * width)
        normed = (x[k].astype(F32) * scale * gain[1:2, cols]).astype(BF16)
        d = jnp.dot(normed, w[cols, :], preferred_element_type=F32)
        acc = d if acc is None else acc + d
    store_gated(gate(acc, taps[1]), out, False)


def back_kernel(halo, gathered, wb, resid, *outs):
    count = gathered.shape[0]
    half = 128
    lefts = []
    for p in range(count // 2):
        a = gathered[2 * p].astype(F32)
        b = gathered[2 * p + 1].astype(F32)
        rows = [
            jnp.concatenate([a[:half, :64], b[:half, :64]], axis=1),
            jnp.concatenate([a[:half, 64:], b[:half, 64:]], axis=1),
        ]
        if halo:
            rows = [jnp.concatenate([a[half:, :64], b[half:, :64]], axis=1)] + rows
        lefts.append(jnp.concatenate(rows, axis=0).astype(BF16))
    left = jnp.concatenate(lefts, axis=1)
    wide = jnp.dot(left, wb[...], preferred_element_type=F32)
    proj = jnp.concatenate(
        [wide[:, k * 128 + 64 : (k + 1) * 128] for k in range(4)], axis=1
    )
    start = resid.shape[0] - proj.shape[0]
    new = (resid[...].astype(F32)[start:] + proj).astype(BF16)
    if halo:
        outs[0][...] = new
        for j in range(count):
            outs[1][j, :, :] = new
    else:
        outs[0][...] = new


def call(kernel, out_shape, n_in, smem=False, scratch=(), flops=0, moved=0):
    specs = ([SMEM] if smem else []) + [VMEM] * (n_in - int(smem))
    return pl.pallas_call(
        kernel,
        out_shape=out_shape,
        in_specs=specs,
        out_specs=jax.tree.map(lambda _: VMEM, out_shape),
        scratch_shapes=scratch,
        cost_estimate=pl.CostEstimate(flops=flops, bytes_accessed=moved, transcendentals=0),
    )


def exchange(block, distance):
    return lax.ppermute(
        block, "sp", [(i, (i + 2 * distance) % 64) for i in range(64)]
    )


def gather_planes(block):
    low = exchange(block, 12)
    high = exchange(block, -12)
    half = ROWS // 2
    up = exchange(jnp.concatenate([block, high, low[:half]], axis=0), 4)
    down = exchange(jnp.concatenate([block, low, high[half:]], axis=0), -4)
    first, second = slice(0, ROWS), slice(ROWS, 2 * ROWS)
    own = jnp.concatenate(
        [up[first], block, low, high, down[first], up[second], down[second]]
        + [up[2 * ROWS :], down[2 * ROWS :]],
        axis=0,
    )
    a = exchange(own, 1)
    b = exchange(own, -1)
    c = exchange(own[: 4 * ROWS], 2)
    d = exchange(own[ROWS : 5 * ROWS], -2)
    mine = jnp.concatenate([own, a, b, c, d], axis=0)
    other = lax.ppermute(mine, "sp", [(i, i ^ 1) for i in range(64)])
    return mine, other


def per_device(tokens, norm_gain, w_outer, w_inner, w_value, w_back, taps):
    count, width = tokens.shape
    feats = w_back.shape[2]
    own = lax.axis_index("tp")
    sp = lax.axis_index("sp")
    pos = jnp.stack([sp // 2, sp % 2]).astype(jnp.int32)
    tp = lax.axis_size("tp")

    packed = pack(w_outer, w_inner, w_value, w_back)
    before = lax.ppermute(tokens[count - HALO :], "sp", [(i, i + 1) for i in range(63)])
    held = [gather_planes(block) for block in packed]

    rows = count + HALO
    resid = lax.dynamic_slice_in_dim(
        jnp.concatenate([before, tokens], axis=0), own * feats, feats, 1
    )
    weights = pltpu.VMEM((width, 256), BF16)
    back_shape = jax.ShapeDtypeStruct((1024, 512), BF16)
    flops = 2 * rows * width * 256
    swap = functools.partial(
        lax.all_to_all, axis_name="tp", split_axis=0, concat_axis=0, tiled=True
    )

    gated, back = call(
        first_kernel,
        [jax.ShapeDtypeStruct((tp, count // 2 + HALO, 128), BF16), back_shape],
        7, True, [weights], flops, 8 << 20,
    )(pos, tokens, before, norm_gain, taps, *held[0])
    whole = swap(gated)
    resid, spread = call(
        functools.partial(back_kernel, True),
        [
            jax.ShapeDtypeStruct((rows, feats), BF16),
            jax.ShapeDtypeStruct((tp, rows, feats), BF16),
        ],
        3, False, [], 2 * rows * 1024 * 512, 4 << 20,
    )(whole, back, resid)
    current = swap(spread)
    gated, back = call(
        second_kernel,
        [jax.ShapeDtypeStruct((tp, count // 2, 128), BF16), back_shape],
        6, True, [weights], flops, 8 << 20,
    )(pos, current, norm_gain, taps, *held[1])
    whole = swap(gated)
    (result,) = call(
        functools.partial(back_kernel, False),
        [jax.ShapeDtypeStruct((count, feats), BF16)],
        3, False, [], 2 * rows * 1024 * 512, 4 << 20,
    )(whole, back, resid)
    return result


def solution(mesh):
    in_specs = (
        P("sp", None),
        P(),
        P(None, "sp", "tp"),
        P(None, "sp", "tp"),
        P(None, "sp", "tp"),
        P(None, "sp", "tp"),
        P(None, None, "tp"),
    )
    out_specs = P("sp", "tp")
    return jax.shard_map(
        per_device, mesh=mesh, in_specs=in_specs, out_specs=out_specs, check_vma=False
    )
```

```python
import functools

import jax
import jax.numpy as jnp
from jax import lax
from jax.experimental import pallas as pl
from jax.experimental.pallas import tpu as pltpu
from jax.sharding import PartitionSpec as P

EPS = 1e-06
HALO = 8
ROWS = 64
VMEM = pl.BlockSpec(memory_space=pltpu.VMEM)
BF16 = jnp.bfloat16
F32 = jnp.float32


def pack_kernel(wo, wi, wv, wb, out):
    for layer in range(out.shape[0]):
        back = wb[layer].astype(F32)
        columns = back.shape[1] // 4
        folded = jnp.concatenate(
            [back[:, k * columns : (k + 1) * columns] for k in range(4)], axis=0
        )
        parts = [w[layer].astype(F32) for w in (wo, wi, wv)] + [folded]
        out[layer] = jnp.concatenate(parts, axis=1).astype(BF16)


def assemble(blocks, w):
    own, own_far, near, near_far = blocks
    sp = lax.axis_index("sp")
    plane, core = lax.rem(lax.div(sp, 2), 4), lax.rem(sp, 2)
    for shift, part, count in ((0, None, 8), (3, 0, 8), (1, 8, 8), (2, 16, 8)):
        residue = lax.rem(plane + shift, 4)
        for side, (first, rest) in enumerate(((own, near), (own_far, near_far))):
            start = 128 * residue + 64 * (core if side == 0 else 1 - core)
            for k in range(count):
                source = first if part is None else rest
                at = (k if part is None else part + k) * ROWS
                row = pl.multiple_of(512 * k + start, 64)
                w[pl.ds(row, ROWS), :] = source[at : at + ROWS, :]


def back_weights(w, wb):
    whole = w[:, 128:].reshape(64, 4, 16, 128)
    for k in range(4):
        wb[:, k * 128 : (k + 1) * 128] = whole[:, k].reshape(1024, 128)


def rounded(v):
    return v.astype(BF16).astype(F32)


def gate(acc, taps):
    outer, inner, value = (rounded(acc[:, k * 64 : (k + 1) * 64]) for k in range(3))
    mixed = rounded(inner * value)
    rows = mixed.shape[0]
    padded = jnp.concatenate([jnp.zeros((8, 64), F32), mixed], axis=0)
    conv = (
        taps[0:1, :] * padded[6 : 6 + rows]
        + taps[1:2, :] * padded[7 : 7 + rows]
        + taps[2:3, :] * padded[8 : 8 + rows]
    )
    return outer * conv


def store_gated(gated, out, halo):
    half = (gated.shape[0] - HALO) // 2
    main = jnp.concatenate(
        [gated[HALO : HALO + half], gated[HALO + half :]], axis=1
    ).astype(BF16)
    copies = out.shape[0]
    if halo:
        extra = jnp.concatenate([gated[:HALO], gated[:HALO]], axis=1).astype(BF16)
    for j in range(copies):
        out[j, :half, :] = main
        if halo:
            out[j, half:, :] = extra


def first_kernel(x, before, gain, taps, own, own_far, near, near_far, out, wb, w):
    assemble((own, own_far, near, near_far), w)
    back_weights(w, wb)
    chunks, width = 16, x.shape[1] // 16
    def part(k):
        cols = slice(k * width, (k + 1) * width)
        return jnp.concatenate(
            [before[:, cols].astype(F32), x[:, cols].astype(F32)], axis=0
        )
    squares = None
    for k in range(chunks):
        p = part(k)
        s = jnp.sum(p * p, axis=1, keepdims=True)
        squares = s if squares is None else squares + s
    scale = lax.rsqrt(squares / x.shape[1] + EPS)
    acc = None
    for k in range(chunks):
        cols = slice(k * width, (k + 1) * width)
        normed = (part(k) * scale * gain[0:1, cols]).astype(BF16)
        d = jnp.dot(normed, w[cols, :], preferred_element_type=F32)
        acc = d if acc is None else acc + d
    store_gated(gate(acc, taps[0]), out, True)


def second_kernel(x, gain, taps, own, own_far, near, near_far, out, wb, w):
    assemble((own, own_far, near, near_far), w)
    back_weights(w, wb)
    chunks, width = x.shape[0], x.shape[2]
    squares = None
    for k in range(chunks):
        p = x[k].astype(F32)
        s = jnp.sum(p * p, axis=1, keepdims=True)
        squares = s if squares is None else squares + s
    scale = lax.rsqrt(squares / (chunks * width) + EPS)
    acc = None
    for k in range(chunks):
        cols = slice(k * width, (k + 1) * width)
        normed = (x[k].astype(F32) * scale * gain[1:2, cols]).astype(BF16)
        d = jnp.dot(normed, w[cols, :], preferred_element_type=F32)
        acc = d if acc is None else acc + d
    store_gated(gate(acc, taps[1]), out, False)


def back_kernel(halo, gathered, wb, resid, *outs):
    count = gathered.shape[0]
    half = 128
    lefts = []
    for p in range(count // 2):
        a = gathered[2 * p].astype(F32)
        b = gathered[2 * p + 1].astype(F32)
        rows = [
            jnp.concatenate([a[:half, :64], b[:half, :64]], axis=1),
            jnp.concatenate([a[:half, 64:], b[:half, 64:]], axis=1),
        ]
        if halo:
            rows = [jnp.concatenate([a[half:, :64], b[half:, :64]], axis=1)] + rows
        lefts.append(jnp.concatenate(rows, axis=0).astype(BF16))
    left = jnp.concatenate(lefts, axis=1)
    wide = jnp.dot(left, wb[...], preferred_element_type=F32)
    proj = jnp.concatenate(
        [wide[:, k * 128 + 64 : (k + 1) * 128] for k in range(4)], axis=1
    )
    start = resid.shape[0] - proj.shape[0]
    new = (resid[...].astype(F32)[start:] + proj).astype(BF16)
    if halo:
        outs[0][...] = new
        for j in range(count):
            outs[1][j, :, :] = new
    else:
        outs[0][...] = new


def call(kernel, out_shape, n_in, scratch=(), flops=0, moved=0):
    return pl.pallas_call(
        kernel,
        out_shape=out_shape,
        in_specs=[VMEM] * n_in,
        out_specs=jax.tree.map(lambda _: VMEM, out_shape),
        scratch_shapes=scratch,
        compiler_params=pltpu.CompilerParams(vmem_limit_bytes=24 << 20),
        cost_estimate=pl.CostEstimate(flops=flops, bytes_accessed=moved, transcendentals=0),
    )


def exchange(block, distance):
    return lax.ppermute(
        block, "sp", [(i, (i + 2 * distance) % 64) for i in range(64)]
    )


def swap_cores(block):
    return lax.ppermute(block, "sp", [(i, i ^ 1) for i in range(64)])


def gather_far(blocks):
    groups = [[r + 8 * k for k in range(8)] for r in range(8)]
    return lax.all_gather(
        blocks, "sp", axis=1, tiled=True, axis_index_groups=groups
    )


def gather_near(own):
    half = own.shape[0] // 2
    own_far = swap_cores(own)
    near = jnp.concatenate(
        [
            exchange(own, 1),
            exchange(own, -1),
            exchange(own[:half], 2),
            exchange(own[half:], -2),
        ],
        axis=0,
    )
    return own, own_far, near, swap_cores(near)


def per_device(tokens, norm_gain, w_outer, w_inner, w_value, w_back, taps):
    count, width = tokens.shape
    feats = w_back.shape[2]
    rank = lax.axis_index("tp")
    tp = lax.axis_size("tp")

    layers, _, mix = w_outer.shape
    packed = call(
        pack_kernel, jax.ShapeDtypeStruct((layers, ROWS, 4 * mix), BF16), 4
    )(w_outer, w_inner, w_value, w_back)
    before = lax.ppermute(tokens[count - HALO :], "sp", [(i, i + 1) for i in range(63)])
    far = gather_far(packed)
    held = [gather_near(far[layer]) for layer in range(layers)]

    rows = count + HALO
    resid = lax.dynamic_slice_in_dim(
        jnp.concatenate([before, tokens], axis=0), rank * feats, feats, 1
    )
    weights = pltpu.VMEM((width, 256), BF16)
    back_shape = jax.ShapeDtypeStruct((1024, 512), BF16)
    flops = 2 * rows * width * 256
    swap = functools.partial(
        lax.all_to_all, axis_name="tp", split_axis=0, concat_axis=0, tiled=True
    )

    gated, back = call(
        first_kernel,
        [jax.ShapeDtypeStruct((tp, count // 2 + HALO, 128), BF16), back_shape],
        8, [weights], flops, 8 << 20,
    )(tokens, before, norm_gain, taps, *held[0])
    whole = swap(gated)
    resid, spread = call(
        functools.partial(back_kernel, True),
        [
            jax.ShapeDtypeStruct((rows, feats), BF16),
            jax.ShapeDtypeStruct((tp, rows, feats), BF16),
        ],
        3, [], 2 * rows * 1024 * 512, 4 << 20,
    )(whole, back, resid)
    current = swap(spread)
    gated, back = call(
        second_kernel,
        [jax.ShapeDtypeStruct((tp, count // 2, 128), BF16), back_shape],
        7, [weights], flops, 8 << 20,
    )(current, norm_gain, taps, *held[1])
    whole = swap(gated)
    (result,) = call(
        functools.partial(back_kernel, False),
        [jax.ShapeDtypeStruct((count, feats), BF16)],
        3, [], 2 * rows * 1024 * 512, 4 << 20,
    )(whole, back, resid)
    return result


def solution(mesh):
    in_specs = (
        P("sp", None),
        P(),
        P(None, "sp", "tp"),
        P(None, "sp", "tp"),
        P(None, "sp", "tp"),
        P(None, "sp", "tp"),
        P(None, None, "tp"),
    )
    out_specs = P("sp", "tp")
    return jax.shard_map(
        per_device, mesh=mesh, in_specs=in_specs, out_specs=out_specs, check_vma=False
    )
```

```python
import functools

import jax
import jax.numpy as jnp
from jax import lax
from jax.experimental import pallas as pl
from jax.experimental.pallas import tpu as pltpu
from jax.sharding import PartitionSpec as P


EPS = 1e-06
HALO = 8
ROWS = 64
VMEM = pl.BlockSpec(memory_space=pltpu.VMEM)
BF16 = jnp.bfloat16
F32 = jnp.float32


def pack_kernel(*refs):
    sources, (out, *held, sems) = refs[:4], refs[4:]
    copies = [
        pltpu.make_async_copy(src, dst, sems.at[i])
        for i, (src, dst) in enumerate(zip(sources, held))
    ]
    for copy in copies:
        copy.start()
    for copy in copies:
        copy.wait()
    for layer in range(out.shape[0]):
        back = held[3][layer].astype(F32)
        columns = back.shape[1] // 4
        folded = jnp.concatenate(
            [back[:, k * columns : (k + 1) * columns] for k in range(4)], axis=0
        )
        parts = [w[layer].astype(F32) for w in held[:3]] + [folded]
        out[layer] = jnp.concatenate(parts, axis=1).astype(BF16)


def pack(*arrays):
    layers, _, mix = arrays[0].shape
    return pl.pallas_call(
        pack_kernel,
        out_shape=jax.ShapeDtypeStruct((layers, ROWS, 4 * mix), BF16),
        in_specs=[pl.BlockSpec(memory_space=pltpu.HBM)] * 4,
        out_specs=VMEM,
        scratch_shapes=[pltpu.VMEM(a.shape, a.dtype) for a in arrays]
        + [pltpu.SemaphoreType.DMA((4,))],
    )(*arrays)


def assemble(blocks, w):
    sp = lax.axis_index("sp")
    plane, core = lax.rem(lax.div(sp, 2), 4), lax.rem(sp, 2)
    far = 1 - core
    down, up = 3 - 2 * core, 1 + 2 * core
    places = (
        ((0, core), (0, far)),
        ((down, core), (down, far), (2, core)),
        ((up, far), (up, core), (2, far)),
    )
    for block, parts in zip(blocks, places):
        for p, (shift, side) in enumerate(parts):
            start = 128 * lax.rem(plane + shift, 4) + 64 * side
            for k in range(8):
                at = (8 * p + k) * ROWS
                row = pl.multiple_of(512 * k + start, 64)
                w[pl.ds(row, ROWS), :] = block[at : at + ROWS, :]


def back_weights(w, wb):
    whole = w[:, 128:].reshape(64, 4, 16, 128)
    parts = [whole[:, k].reshape(1024, 128)[:, 64:] for k in range(4)]
    wb[...] = jnp.concatenate(parts, axis=1)


def rounded(v):
    return v.astype(BF16).astype(F32)


def gate(acc, taps):
    outer, inner, value = (rounded(acc[:, k * 64 : (k + 1) * 64]) for k in range(3))
    mixed = rounded(inner * value)
    rows = mixed.shape[0]
    padded = jnp.concatenate([jnp.zeros((8, 64), F32), mixed], axis=0)
    conv = (
        taps[0:1, :] * padded[6 : 6 + rows]
        + taps[1:2, :] * padded[7 : 7 + rows]
        + taps[2:3, :] * padded[8 : 8 + rows]
    )
    return outer * conv


def store_gated(gated, out, halo):
    half = (gated.shape[0] - HALO) // 2
    main = jnp.concatenate(
        [gated[HALO : HALO + half], gated[HALO + half :]], axis=1
    ).astype(BF16)
    copies = out.shape[0]
    if halo:
        extra = jnp.concatenate([gated[:HALO], gated[:HALO]], axis=1).astype(BF16)
    for j in range(copies):
        out[j, :half, :] = main
        if halo:
            out[j, half:, :] = extra


def first_kernel(x, before, gain, taps, own, near, near_far, out, wb, w):
    assemble((own, near, near_far), w)
    back_weights(w, wb)
    chunks, width = 16, x.shape[1] // 16
    def part(k):
        cols = slice(k * width, (k + 1) * width)
        return jnp.concatenate(
            [before[:, cols].astype(F32), x[:, cols].astype(F32)], axis=0
        )
    squares = None
    for k in range(chunks):
        p = part(k)
        s = jnp.sum(p * p, axis=1, keepdims=True)
        squares = s if squares is None else squares + s
    scale = lax.rsqrt(squares / x.shape[1] + EPS)
    acc = None
    for k in range(chunks):
        cols = slice(k * width, (k + 1) * width)
        normed = (part(k) * scale * gain[0:1, cols]).astype(BF16)
        d = jnp.dot(normed, w[cols, :], preferred_element_type=F32)
        acc = d if acc is None else acc + d
    store_gated(gate(acc, taps[0]), out, True)


def second_kernel(x, gain, taps, own, near, near_far, out, wb, w):
    assemble((own, near, near_far), w)
    back_weights(w, wb)
    chunks, width = x.shape[0], x.shape[2]
    squares = None
    for k in range(chunks):
        p = x[k].astype(F32)
        s = jnp.sum(p * p, axis=1, keepdims=True)
        squares = s if squares is None else squares + s
    scale = lax.rsqrt(squares / (chunks * width) + EPS)
    acc = None
    for k in range(chunks):
        cols = slice(k * width, (k + 1) * width)
        normed = (x[k].astype(F32) * scale * gain[1:2, cols]).astype(BF16)
        d = jnp.dot(normed, w[cols, :], preferred_element_type=F32)
        acc = d if acc is None else acc + d
    store_gated(gate(acc, taps[1]), out, False)


def back_kernel(halo, gathered, wb, resid, *outs):
    count = gathered.shape[0]
    half = 128
    lefts = []
    for p in range(count // 2):
        a = gathered[2 * p].astype(F32)
        b = gathered[2 * p + 1].astype(F32)
        rows = [
            jnp.concatenate([a[:half, :64], b[:half, :64]], axis=1),
            jnp.concatenate([a[:half, 64:], b[:half, 64:]], axis=1),
        ]
        if halo:
            rows = [jnp.concatenate([a[half:, :64], b[half:, :64]], axis=1)] + rows
        lefts.append(jnp.concatenate(rows, axis=0).astype(BF16))
    left = jnp.concatenate(lefts, axis=1)
    proj = jnp.dot(left, wb[...], preferred_element_type=F32)
    start = resid.shape[0] - proj.shape[0]
    new = (resid[...].astype(F32)[start:] + proj).astype(BF16)
    if halo:
        outs[0][...] = new
        for j in range(count):
            outs[1][j, :, :] = new
    else:
        outs[0][...] = new


def call(kernel, out_shape, n_in, scratch=(), flops=0, moved=0):
    return pl.pallas_call(
        kernel,
        out_shape=out_shape,
        in_specs=[VMEM] * n_in,
        out_specs=jax.tree.map(lambda _: VMEM, out_shape),
        scratch_shapes=scratch,
        compiler_params=pltpu.CompilerParams(vmem_limit_bytes=24 << 20),
        cost_estimate=pl.CostEstimate(flops=flops, bytes_accessed=moved, transcendentals=0),
    )


def exchange(block, distance):
    step = [2 * distance, -2 * distance]
    return lax.ppermute(block, "sp", [(i, (i + step[i % 2]) % 64) for i in range(64)])


def swap_cores(block):
    return lax.ppermute(block, "sp", [(i, i ^ 1) for i in range(64)])


def gather_far(blocks):
    groups = [[r + 8 * k for k in range(8)] for r in range(8)]
    return lax.all_gather(
        blocks, "sp", axis=1, tiled=True, axis_index_groups=groups
    )


def per_device(tokens, norm_gain, w_outer, w_inner, w_value, w_back, taps):
    count, width = tokens.shape
    feats = w_back.shape[2]
    rank = lax.axis_index("tp")
    tp = lax.axis_size("tp")
    layers = w_outer.shape[0]
    rows = count + HALO

    packed = pack(w_outer, w_inner, w_value, w_back)
    before = lax.ppermute(tokens[count - HALO :], "sp", [(i, i + 1) for i in range(63)])
    far = gather_far(packed)
    twos = []
    for layer in range(layers):
        twos.append(exchange(far[layer], 2))
    partner = swap_cores(far)
    held = []
    for layer in range(layers):
        both = jnp.concatenate([far[layer], partner[layer]], axis=0)
        one = exchange(both, 1)
        near = jnp.concatenate([one, twos[layer]], axis=0)
        if layer == 0:
            resid = lax.dynamic_slice_in_dim(
                jnp.concatenate([before, tokens], axis=0), rank * feats, feats, 1
            )
            near, before, resid = lax.optimization_barrier((near, before, resid))
        held.append((both, near, swap_cores(near)))

    weights = pltpu.VMEM((width, 256), BF16)
    back_shape = jax.ShapeDtypeStruct((1024, 256), BF16)
    flops = 2 * rows * width * 256
    send = functools.partial(
        lax.all_to_all, axis_name="tp", split_axis=0, concat_axis=0, tiled=True
    )

    gated, back = call(
        first_kernel,
        [jax.ShapeDtypeStruct((tp, count // 2 + HALO, 128), BF16), back_shape],
        7, [weights], flops, 8 << 20,
    )(tokens, before, norm_gain, taps, *held[0])
    whole = send(gated)
    resid, spread = call(
        functools.partial(back_kernel, True),
        [
            jax.ShapeDtypeStruct((rows, feats), BF16),
            jax.ShapeDtypeStruct((tp, rows, feats), BF16),
        ],
        3, [], 2 * rows * 1024 * 256, 4 << 20,
    )(whole, back, resid)
    current = send(spread)
    gated, back = call(
        second_kernel,
        [jax.ShapeDtypeStruct((tp, count // 2, 128), BF16), back_shape],
        6, [weights], flops, 8 << 20,
    )(current, norm_gain, taps, *held[1])
    whole = send(gated)
    (result,) = call(
        functools.partial(back_kernel, False),
        [jax.ShapeDtypeStruct((count, feats), BF16)],
        3, [], 2 * rows * 1024 * 256, 4 << 20,
    )(whole, back, resid)
    return result


def solution(mesh):
    in_specs = (
        P("sp", None),
        P(),
        P(None, "sp", "tp"),
        P(None, "sp", "tp"),
        P(None, "sp", "tp"),
        P(None, "sp", "tp"),
        P(None, None, "tp"),
    )
    out_specs = P("sp", "tp")
    return jax.shard_map(
        per_device, mesh=mesh, in_specs=in_specs, out_specs=out_specs, check_vma=False
    )
```

```python
import functools

import jax
import jax.numpy as jnp
from jax import lax
from jax.experimental import pallas as pl
from jax.experimental.pallas import tpu as pltpu
from jax.sharding import PartitionSpec as P


EPS = 1e-06
HALO = 8
ROWS = 64
VMEM = pl.BlockSpec(memory_space=pltpu.VMEM)
BF16 = jnp.bfloat16
F32 = jnp.float32


def pack_kernel(*refs):
    sources, (out, *held, sems) = refs[:4], refs[4:]
    copies = [
        pltpu.make_async_copy(src, dst, sems.at[i])
        for i, (src, dst) in enumerate(zip(sources, held))
    ]
    for copy in copies:
        copy.start()
    for copy in copies:
        copy.wait()
    for layer in range(out.shape[0]):
        back = held[3][layer].astype(F32)
        columns = back.shape[1] // 4
        folded = jnp.concatenate(
            [back[:, k * columns : (k + 1) * columns] for k in range(4)], axis=0
        )
        parts = [w[layer].astype(F32) for w in held[:3]] + [folded]
        out[layer] = jnp.concatenate(parts, axis=1).astype(BF16)


def pack(*arrays):
    layers, _, mix = arrays[0].shape
    return pl.pallas_call(
        pack_kernel,
        out_shape=jax.ShapeDtypeStruct((layers, ROWS, 4 * mix), BF16),
        in_specs=[pl.BlockSpec(memory_space=pltpu.HBM)] * 4,
        out_specs=VMEM,
        scratch_shapes=[pltpu.VMEM(a.shape, a.dtype) for a in arrays]
        + [pltpu.SemaphoreType.DMA((4,))],
    )(*arrays)


def assemble(blocks, w):
    sp = lax.axis_index("sp")
    plane, core = lax.rem(lax.div(sp, 2), 4), lax.rem(sp, 2)
    far = 1 - core
    down, up = 3 - 2 * core, 1 + 2 * core
    places = (
        ((0, core), (0, far)),
        ((down, core), (down, far), (2, core)),
        ((up, far), (up, core), (2, far)),
    )
    for block, parts in zip(blocks, places):
        for p, (shift, side) in enumerate(parts):
            start = 128 * lax.rem(plane + shift, 4) + 64 * side
            for k in range(8):
                at = (8 * p + k) * ROWS
                row = pl.multiple_of(512 * k + start, 64)
                w[pl.ds(row, ROWS), :] = block[at : at + ROWS, :]


def back_weights(w, wb):
    whole = w[:, 128:].reshape(64, 4, 16, 128)
    parts = [whole[:, k].reshape(1024, 128)[:, 64:] for k in range(4)]
    wb[...] = jnp.concatenate(parts, axis=1)


def rounded(v):
    return v.astype(BF16).astype(F32)


def gate(acc, taps):
    outer, inner, value = (rounded(acc[:, k * 64 : (k + 1) * 64]) for k in range(3))
    mixed = rounded(inner * value)
    rows = mixed.shape[0]
    padded = jnp.concatenate([jnp.zeros((8, 64), F32), mixed], axis=0)
    conv = (
        taps[0:1, :] * padded[6 : 6 + rows]
        + taps[1:2, :] * padded[7 : 7 + rows]
        + taps[2:3, :] * padded[8 : 8 + rows]
    )
    return outer * conv


def store_gated(gated, out, halo):
    half = (gated.shape[0] - HALO) // 2
    main = jnp.concatenate(
        [gated[HALO : HALO + half], gated[HALO + half :]], axis=1
    ).astype(BF16)
    copies = out.shape[0]
    if halo:
        extra = jnp.concatenate([gated[:HALO], gated[:HALO]], axis=1).astype(BF16)
    for j in range(copies):
        out[j, :half, :] = main
        if halo:
            out[j, half:, :] = extra


def first_kernel(x, before, gain, taps, own, near, near_far, out, wb, w):
    assemble((own, near, near_far), w)
    back_weights(w, wb)
    chunks, width = 16, x.shape[1] // 16
    def part(k):
        cols = slice(k * width, (k + 1) * width)
        return jnp.concatenate(
            [before[:, cols].astype(F32), x[:, cols].astype(F32)], axis=0
        )
    squares = None
    for k in range(chunks):
        p = part(k)
        s = jnp.sum(p * p, axis=1, keepdims=True)
        squares = s if squares is None else squares + s
    scale = lax.rsqrt(squares / x.shape[1] + EPS)
    acc = None
    for k in range(chunks):
        cols = slice(k * width, (k + 1) * width)
        normed = (part(k) * scale * gain[0:1, cols]).astype(BF16)
        d = jnp.dot(normed, w[cols, :], preferred_element_type=F32)
        acc = d if acc is None else acc + d
    store_gated(gate(acc, taps[0]), out, True)


def scale_kernel(x, out):
    chunks, _, width = x.shape
    squares = None
    for k in range(chunks):
        p = x[k].astype(F32)
        s = jnp.sum(p * p, axis=1, keepdims=True)
        squares = s if squares is None else squares + s
    out[...] = lax.rsqrt(squares / (chunks * width) + EPS)


def second_kernel(x, scale, gain, taps, own, near, near_far, out, wb, w):
    assemble((own, near, near_far), w)
    back_weights(w, wb)
    chunks, width = x.shape[0], x.shape[2]
    acc = None
    for k in range(chunks):
        cols = slice(k * width, (k + 1) * width)
        normed = (x[k].astype(F32) * scale[...] * gain[1:2, cols]).astype(BF16)
        d = jnp.dot(normed, w[cols, :], preferred_element_type=F32)
        acc = d if acc is None else acc + d
    store_gated(gate(acc, taps[1]), out, False)


def back_kernel(halo, gathered, wb, resid, *outs):
    count = gathered.shape[0]
    half = 128
    lefts = []
    for p in range(count // 2):
        a = gathered[2 * p].astype(F32)
        b = gathered[2 * p + 1].astype(F32)
        rows = [
            jnp.concatenate([a[:half, :64], b[:half, :64]], axis=1),
            jnp.concatenate([a[:half, 64:], b[:half, 64:]], axis=1),
        ]
        if halo:
            rows = [jnp.concatenate([a[half:, :64], b[half:, :64]], axis=1)] + rows
        lefts.append(jnp.concatenate(rows, axis=0).astype(BF16))
    left = jnp.concatenate(lefts, axis=1)
    proj = jnp.dot(left, wb[...], preferred_element_type=F32)
    start = resid.shape[0] - proj.shape[0]
    new = (resid[...].astype(F32)[start:] + proj).astype(BF16)
    if halo:
        outs[0][...] = new
        for j in range(count):
            outs[1][j, :, :] = new
    else:
        outs[0][...] = new


def call(kernel, out_shape, n_in, scratch=(), flops=0, moved=0):
    return pl.pallas_call(
        kernel,
        out_shape=out_shape,
        in_specs=[VMEM] * n_in,
        out_specs=jax.tree.map(lambda _: VMEM, out_shape),
        scratch_shapes=scratch,
        compiler_params=pltpu.CompilerParams(vmem_limit_bytes=24 << 20),
        cost_estimate=pl.CostEstimate(flops=flops, bytes_accessed=moved, transcendentals=0),
    )


def exchange(block, distance):
    step = [2 * distance, -2 * distance]
    return lax.ppermute(block, "sp", [(i, (i + step[i % 2]) % 64) for i in range(64)])


def swap_cores(block):
    return lax.ppermute(block, "sp", [(i, i ^ 1) for i in range(64)])


def gather_far(blocks):
    groups = [[r + 8 * k for k in range(8)] for r in range(8)]
    return lax.all_gather(
        blocks, "sp", axis=1, tiled=True, axis_index_groups=groups
    )


def per_device(tokens, norm_gain, w_outer, w_inner, w_value, w_back, taps):
    count, width = tokens.shape
    feats = w_back.shape[2]
    rank = lax.axis_index("tp")
    tp = lax.axis_size("tp")
    layers = w_outer.shape[0]
    rows = count + HALO

    packed = pack(w_outer, w_inner, w_value, w_back)
    before = lax.ppermute(tokens[count - HALO :], "sp", [(i, i + 1) for i in range(63)])
    far = gather_far(packed)
    twos = []
    for layer in range(layers):
        twos.append(exchange(far[layer], 2))
    partner = swap_cores(far)
    held = []
    for layer in range(layers):
        both = jnp.concatenate([far[layer], partner[layer]], axis=0)
        one = exchange(both, 1)
        near = jnp.concatenate([one, twos[layer]], axis=0)
        if layer == 0:
            resid = lax.dynamic_slice_in_dim(
                jnp.concatenate([before, tokens], axis=0), rank * feats, feats, 1
            )
            near, before, resid = lax.optimization_barrier((near, before, resid))
        held.append((both, near, swap_cores(near)))

    weights = pltpu.VMEM((width, 256), BF16)
    back_shape = jax.ShapeDtypeStruct((1024, 256), BF16)
    flops = 2 * rows * width * 256
    send = functools.partial(
        lax.all_to_all, axis_name="tp", split_axis=0, concat_axis=0, tiled=True
    )

    gated, back = call(
        first_kernel,
        [jax.ShapeDtypeStruct((tp, count // 2 + HALO, 128), BF16), back_shape],
        7, [weights], flops, 8 << 20,
    )(tokens, before, norm_gain, taps, *held[0])
    whole = send(gated)
    resid, spread = call(
        functools.partial(back_kernel, True),
        [
            jax.ShapeDtypeStruct((rows, feats), BF16),
            jax.ShapeDtypeStruct((tp, rows, feats), BF16),
        ],
        3, [], 2 * rows * 1024 * 256, 4 << 20,
    )(whole, back, resid)
    current = send(spread)
    scale = call(
        scale_kernel, jax.ShapeDtypeStruct((rows, 1), F32), 1, [], 3 * rows * width, 2 << 20
    )(current)
    gated, back = call(
        second_kernel,
        [jax.ShapeDtypeStruct((tp, count // 2, 128), BF16), back_shape],
        7, [weights], flops, 8 << 20,
    )(current, scale, norm_gain, taps, *held[1])
    whole = send(gated)
    (result,) = call(
        functools.partial(back_kernel, False),
        [jax.ShapeDtypeStruct((count, feats), BF16)],
        3, [], 2 * rows * 1024 * 256, 4 << 20,
    )(whole, back, resid)
    return result


def solution(mesh):
    in_specs = (
        P("sp", None),
        P(),
        P(None, "sp", "tp"),
        P(None, "sp", "tp"),
        P(None, "sp", "tp"),
        P(None, "sp", "tp"),
        P(None, None, "tp"),
    )
    out_specs = P("sp", "tp")
    return jax.shard_map(
        per_device, mesh=mesh, in_specs=in_specs, out_specs=out_specs, check_vma=False
    )
```

```python
import functools

import jax
import jax.numpy as jnp
from jax import lax
from jax.experimental import pallas as pl
from jax.experimental.pallas import tpu as pltpu
from jax.sharding import PartitionSpec as P


EPS = 1e-06
HALO = 8
ROWS = 64
VMEM = pl.BlockSpec(memory_space=pltpu.VMEM)
BF16 = jnp.bfloat16
F32 = jnp.float32


def pack_kernel(*refs):
    sources, (out, *held, sems) = refs[:4], refs[4:]
    copies = [
        pltpu.make_async_copy(src, dst, sems.at[i])
        for i, (src, dst) in enumerate(zip(sources, held))
    ]
    for copy in copies:
        copy.start()
    for copy in copies:
        copy.wait()
    for layer in range(out.shape[0]):
        back = held[3][layer].astype(F32)
        columns = back.shape[1] // 4
        folded = jnp.concatenate(
            [back[:, k * columns : (k + 1) * columns] for k in range(4)], axis=0
        )
        parts = [w[layer].astype(F32) for w in held[:3]] + [folded]
        out[layer] = jnp.concatenate(parts, axis=1).astype(BF16)


def pack(*arrays):
    layers, _, mix = arrays[0].shape
    return pl.pallas_call(
        pack_kernel,
        out_shape=jax.ShapeDtypeStruct((layers, ROWS, 4 * mix), BF16),
        in_specs=[pl.BlockSpec(memory_space=pltpu.HBM)] * 4,
        out_specs=VMEM,
        scratch_shapes=[pltpu.VMEM(a.shape, a.dtype) for a in arrays]
        + [pltpu.SemaphoreType.DMA((4,))],
    )(*arrays)


def assemble(blocks, w):
    sp = lax.axis_index("sp")
    plane, core = lax.rem(lax.div(sp, 2), 4), lax.rem(sp, 2)
    far = 1 - core
    down, up = 3 - 2 * core, 1 + 2 * core
    places = (
        ((0, core), (0, far)),
        ((down, core), (down, far), (2, core)),
        ((up, far), (up, core), (2, far)),
    )
    for block, parts in zip(blocks, places):
        for p, (shift, side) in enumerate(parts):
            start = 128 * lax.rem(plane + shift, 4) + 64 * side
            for k in range(8):
                at = (8 * p + k) * ROWS
                row = pl.multiple_of(512 * k + start, 64)
                w[pl.ds(row, ROWS), :] = block[at : at + ROWS, :]


def back_weights(w, wb):
    whole = w[:, 128:].reshape(64, 4, 16, 128)
    parts = [whole[:, k].reshape(1024, 128)[:, 64:] for k in range(4)]
    wb[...] = jnp.concatenate(parts, axis=1)


def rounded(v):
    return v.astype(BF16).astype(F32)


def gate(acc, taps):
    outer, inner, value = (rounded(acc[:, k * 64 : (k + 1) * 64]) for k in range(3))
    mixed = rounded(inner * value)
    rows = mixed.shape[0]
    padded = jnp.concatenate([jnp.zeros((8, 64), F32), mixed], axis=0)
    conv = (
        taps[0:1, :] * padded[6 : 6 + rows]
        + taps[1:2, :] * padded[7 : 7 + rows]
        + taps[2:3, :] * padded[8 : 8 + rows]
    )
    return outer * conv


def store_gated(gated, out, halo):
    half = (gated.shape[0] - HALO) // 2
    main = jnp.concatenate(
        [gated[HALO : HALO + half], gated[HALO + half :]], axis=1
    ).astype(BF16)
    copies = out.shape[0]
    if halo:
        extra = jnp.concatenate([gated[:HALO], gated[:HALO]], axis=1).astype(BF16)
    for j in range(copies):
        out[j, :half, :] = main
        if halo:
            out[j, half:, :] = extra


def first_kernel(x, before, gain, taps, own, near, near_far, out, wb, w):
    assemble((own, near, near_far), w)
    back_weights(w, wb)
    chunks, width = 16, x.shape[1] // 16
    def part(k):
        cols = slice(k * width, (k + 1) * width)
        return jnp.concatenate(
            [before[:, cols].astype(F32), x[:, cols].astype(F32)], axis=0
        )
    squares = None
    for k in range(chunks):
        p = part(k)
        s = jnp.sum(p * p, axis=1, keepdims=True)
        squares = s if squares is None else squares + s
    scale = lax.rsqrt(squares / x.shape[1] + EPS)
    acc = None
    for k in range(chunks):
        cols = slice(k * width, (k + 1) * width)
        normed = (part(k) * scale * gain[0:1, cols]).astype(BF16)
        d = jnp.dot(normed, w[cols, :], preferred_element_type=F32)
        acc = d if acc is None else acc + d
    store_gated(gate(acc, taps[0]), out, True)


def second_kernel(x, gain, taps, own, near, near_far, out, wb, resid, w):
    resid[...] = x[lax.axis_index("tp")]
    assemble((own, near, near_far), w)
    back_weights(w, wb)
    chunks, width = x.shape[0], x.shape[2]
    squares = None
    for k in range(chunks):
        p = x[k].astype(F32)
        s = jnp.sum(p * p, axis=1, keepdims=True)
        squares = s if squares is None else squares + s
    scale = lax.rsqrt(squares / (chunks * width) + EPS)
    acc = None
    for k in range(chunks):
        cols = slice(k * width, (k + 1) * width)
        normed = (x[k].astype(F32) * scale * gain[1:2, cols]).astype(BF16)
        d = jnp.dot(normed, w[cols, :], preferred_element_type=F32)
        acc = d if acc is None else acc + d
    store_gated(gate(acc, taps[1]), out, False)


def back_kernel(halo, gathered, wb, resid, *outs):
    count = gathered.shape[0]
    half = 128
    lefts = []
    for p in range(count // 2):
        a = gathered[2 * p].astype(F32)
        b = gathered[2 * p + 1].astype(F32)
        rows = [
            jnp.concatenate([a[:half, :64], b[:half, :64]], axis=1),
            jnp.concatenate([a[:half, 64:], b[:half, 64:]], axis=1),
        ]
        if halo:
            rows = [jnp.concatenate([a[half:, :64], b[half:, :64]], axis=1)] + rows
        lefts.append(jnp.concatenate(rows, axis=0).astype(BF16))
    left = jnp.concatenate(lefts, axis=1)
    proj = jnp.dot(left, wb[...], preferred_element_type=F32)
    start = resid.shape[0] - proj.shape[0]
    new = (resid[...].astype(F32)[start:] + proj).astype(BF16)
    if halo:
        for j in range(count):
            outs[0][j, :, :] = new
    else:
        outs[0][...] = new


def call(kernel, out_shape, n_in, scratch=(), flops=0, moved=0):
    return pl.pallas_call(
        kernel,
        out_shape=out_shape,
        in_specs=[VMEM] * n_in,
        out_specs=jax.tree.map(lambda _: VMEM, out_shape),
        scratch_shapes=scratch,
        compiler_params=pltpu.CompilerParams(vmem_limit_bytes=24 << 20),
        cost_estimate=pl.CostEstimate(flops=flops, bytes_accessed=moved, transcendentals=0),
    )


def exchange(block, distance):
    step = [2 * distance, -2 * distance]
    return lax.ppermute(block, "sp", [(i, (i + step[i % 2]) % 64) for i in range(64)])


def swap_cores(block):
    return lax.ppermute(block, "sp", [(i, i ^ 1) for i in range(64)])


def gather_far(blocks):
    groups = [[r + 8 * k for k in range(8)] for r in range(8)]
    flat = blocks.reshape(-1, blocks.shape[2])
    return lax.all_gather(flat, "sp", axis=0, tiled=True, axis_index_groups=groups)


def layer_of(far, layer):
    parts = far.reshape(8, -1, ROWS, far.shape[1])
    return parts[:, layer].reshape(-1, far.shape[1])


def per_device(tokens, norm_gain, w_outer, w_inner, w_value, w_back, taps):
    count, width = tokens.shape
    feats = w_back.shape[2]
    rank = lax.axis_index("tp")
    tp = lax.axis_size("tp")
    layers = w_outer.shape[0]
    rows = count + HALO

    packed = pack(w_outer, w_inner, w_value, w_back)
    before = lax.ppermute(tokens[count - HALO :], "sp", [(i, i + 1) for i in range(63)])
    far = gather_far(packed)
    twos = []
    for layer in range(layers):
        twos.append(exchange(layer_of(far, layer), 2))
    partner = swap_cores(far)
    held = []
    for layer in range(layers):
        both = jnp.concatenate([layer_of(far, layer), layer_of(partner, layer)], axis=0)
        one = exchange(both, 1)
        near = jnp.concatenate([one, twos[layer]], axis=0)
        if layer == 0:
            resid = lax.dynamic_slice_in_dim(
                jnp.concatenate([before, tokens], axis=0), rank * feats, feats, 1
            )
            near, before, resid = lax.optimization_barrier((near, before, resid))
        held.append((both, near, swap_cores(near)))

    weights = pltpu.VMEM((width, 256), BF16)
    back_shape = jax.ShapeDtypeStruct((1024, 256), BF16)
    flops = 2 * rows * width * 256
    send = functools.partial(
        lax.all_to_all, axis_name="tp", split_axis=0, concat_axis=0, tiled=True
    )

    gated, back = call(
        first_kernel,
        [jax.ShapeDtypeStruct((tp, count // 2 + HALO, 128), BF16), back_shape],
        7, [weights], flops, 8 << 20,
    )(tokens, before, norm_gain, taps, *held[0])
    whole = send(gated)
    (spread,) = call(
        functools.partial(back_kernel, True),
        [jax.ShapeDtypeStruct((tp, rows, feats), BF16)],
        3, [], 2 * rows * 1024 * 256, 4 << 20,
    )(whole, back, resid)
    current = send(spread)
    gated, back, resid = call(
        second_kernel,
        [
            jax.ShapeDtypeStruct((tp, count // 2, 128), BF16),
            back_shape,
            jax.ShapeDtypeStruct((rows, feats), BF16),
        ],
        6, [weights], flops, 8 << 20,
    )(current, norm_gain, taps, *held[1])
    whole = send(gated)
    (result,) = call(
        functools.partial(back_kernel, False),
        [jax.ShapeDtypeStruct((count, feats), BF16)],
        3, [], 2 * rows * 1024 * 256, 4 << 20,
    )(whole, back, resid)
    return result


def solution(mesh):
    in_specs = (
        P("sp", None),
        P(),
        P(None, "sp", "tp"),
        P(None, "sp", "tp"),
        P(None, "sp", "tp"),
        P(None, "sp", "tp"),
        P(None, None, "tp"),
    )
    out_specs = P("sp", "tp")
    return jax.shard_map(
        per_device, mesh=mesh, in_specs=in_specs, out_specs=out_specs, check_vma=False
    )
```

```python
import functools

import jax
import jax.numpy as jnp
from jax import lax
from jax.experimental import pallas as pl
from jax.experimental.pallas import tpu as pltpu
from jax.sharding import PartitionSpec as P


EPS = 1e-06
HALO = 8
ROWS = 64
VMEM = pl.BlockSpec(memory_space=pltpu.VMEM)
BF16 = jnp.bfloat16
F32 = jnp.float32


def pack_kernel(*refs):
    sources, (out, *held, sems) = refs[:4], refs[4:]
    copies = [
        pltpu.make_async_copy(src, dst, sems.at[i])
        for i, (src, dst) in enumerate(zip(sources, held))
    ]
    for copy in copies:
        copy.start()
    for copy in copies:
        copy.wait()
    for layer in range(out.shape[0]):
        back = held[3][layer].astype(F32)
        columns = back.shape[1] // 4
        folded = jnp.concatenate(
            [back[:, k * columns : (k + 1) * columns] for k in range(4)], axis=0
        )
        parts = [w[layer].astype(F32) for w in held[:3]] + [folded]
        out[layer] = jnp.concatenate(parts, axis=1).astype(BF16)


def pack(*arrays):
    layers, _, mix = arrays[0].shape
    return pl.pallas_call(
        pack_kernel,
        out_shape=jax.ShapeDtypeStruct((layers, ROWS, 4 * mix), BF16),
        in_specs=[pl.BlockSpec(memory_space=pltpu.HBM)] * 4,
        out_specs=VMEM,
        scratch_shapes=[pltpu.VMEM(a.shape, a.dtype) for a in arrays]
        + [pltpu.SemaphoreType.DMA((4,))],
    )(*arrays)


def assemble(blocks, w):
    sp = lax.axis_index("sp")
    plane, core = lax.rem(lax.div(sp, 2), 4), lax.rem(sp, 2)
    far = 1 - core
    down, up = 3 - 2 * core, 1 + 2 * core
    places = (
        ((0, core), (0, far)),
        ((down, core), (down, far), (2, core)),
        ((up, far), (up, core), (2, far)),
    )
    for block, parts in zip(blocks, places):
        for p, (shift, side) in enumerate(parts):
            start = 128 * lax.rem(plane + shift, 4) + 64 * side
            for k in range(8):
                at = (8 * p + k) * ROWS
                row = pl.multiple_of(512 * k + start, 64)
                w[pl.ds(row, ROWS), :] = block[at : at + ROWS, :]


def back_weights(w, wb):
    whole = w[:, 128:].reshape(64, 4, 16, 128)
    parts = [whole[:, k].reshape(1024, 128)[:, 64:] for k in range(4)]
    wb[...] = jnp.concatenate(parts, axis=1)


def rounded(v):
    return v.astype(BF16).astype(F32)


def gate(acc, taps):
    outer, inner, value = (rounded(acc[:, k * 64 : (k + 1) * 64]) for k in range(3))
    mixed = rounded(inner * value)
    rows = mixed.shape[0]
    padded = jnp.concatenate([jnp.zeros((8, 64), F32), mixed], axis=0)
    conv = (
        taps[0:1, :] * padded[6 : 6 + rows]
        + taps[1:2, :] * padded[7 : 7 + rows]
        + taps[2:3, :] * padded[8 : 8 + rows]
    )
    return outer * conv


def store_gated(gated, out, halo):
    half = (gated.shape[0] - HALO) // 2
    main = jnp.concatenate(
        [gated[HALO : HALO + half], gated[HALO + half :]], axis=1
    ).astype(BF16)
    copies = out.shape[0]
    if halo:
        extra = jnp.concatenate([gated[:HALO], gated[:HALO]], axis=1).astype(BF16)
    for j in range(copies):
        out[j, :half, :] = main
        if halo:
            out[j, half:, :] = extra


def first_kernel(x, before, gain, taps, own, near, near_far, out, wb, w):
    assemble((own, near, near_far), w)
    back_weights(w, wb)
    chunks, width = 16, x.shape[1] // 16
    def part(k):
        cols = slice(k * width, (k + 1) * width)
        return jnp.concatenate(
            [before[:, cols].astype(F32), x[:, cols].astype(F32)], axis=0
        )
    squares = None
    for k in range(chunks):
        p = part(k)
        s = jnp.sum(p * p, axis=1, keepdims=True)
        squares = s if squares is None else squares + s
    scale = lax.rsqrt(squares / x.shape[1] + EPS)
    acc = None
    for k in range(chunks):
        cols = slice(k * width, (k + 1) * width)
        normed = (part(k) * scale * gain[0:1, cols]).astype(BF16)
        d = jnp.dot(normed, w[cols, :], preferred_element_type=F32)
        acc = d if acc is None else acc + d
    store_gated(gate(acc, taps[0]), out, True)


def second_kernel(x, gain, taps, own, near, near_far, out, wb, resid, w):
    resid[...] = x[lax.axis_index("tp")]
    assemble((own, near, near_far), w)
    back_weights(w, wb)
    chunks, width = x.shape[0], x.shape[2]
    squares = None
    for k in range(chunks):
        p = x[k].astype(F32)
        s = jnp.sum(p * p, axis=1, keepdims=True)
        squares = s if squares is None else squares + s
    scale = lax.rsqrt(squares / (chunks * width) + EPS)
    acc = None
    for k in range(chunks):
        cols = slice(k * width, (k + 1) * width)
        normed = (x[k].astype(F32) * scale * gain[1:2, cols]).astype(BF16)
        d = jnp.dot(normed, w[cols, :], preferred_element_type=F32)
        acc = d if acc is None else acc + d
    store_gated(gate(acc, taps[1]), out, False)


def back_kernel(halo, gathered, wb, resid, *outs):
    count = gathered.shape[0]
    half = 128
    lefts = []
    for p in range(count // 2):
        a = gathered[2 * p].astype(F32)
        b = gathered[2 * p + 1].astype(F32)
        rows = [
            jnp.concatenate([a[:half, :64], b[:half, :64]], axis=1),
            jnp.concatenate([a[:half, 64:], b[:half, 64:]], axis=1),
        ]
        if halo:
            rows = [jnp.concatenate([a[half:, :64], b[half:, :64]], axis=1)] + rows
        lefts.append(jnp.concatenate(rows, axis=0).astype(BF16))
    left = jnp.concatenate(lefts, axis=1)
    proj = jnp.dot(left, wb[...], preferred_element_type=F32)
    start = resid.shape[0] - proj.shape[0]
    new = (resid[...].astype(F32)[start:] + proj).astype(BF16)
    if halo:
        spread, block, sems = outs
        block[...] = new
        copies = [
            pltpu.make_async_copy(block, spread.at[j], sems.at[j]) for j in range(count)
        ]
        for copy in copies:
            copy.start()
        for copy in copies:
            copy.wait()
    else:
        outs[0][...] = new


def call(kernel, out_shape, n_in, scratch=(), flops=0, moved=0):
    return pl.pallas_call(
        kernel,
        out_shape=out_shape,
        in_specs=[VMEM] * n_in,
        out_specs=jax.tree.map(lambda _: VMEM, out_shape),
        scratch_shapes=scratch,
        compiler_params=pltpu.CompilerParams(vmem_limit_bytes=24 << 20),
        cost_estimate=pl.CostEstimate(flops=flops, bytes_accessed=moved, transcendentals=0),
    )


def exchange(block, distance):
    step = [2 * distance, -2 * distance]
    return lax.ppermute(block, "sp", [(i, (i + step[i % 2]) % 64) for i in range(64)])


def swap_cores(block):
    return lax.ppermute(block, "sp", [(i, i ^ 1) for i in range(64)])


def gather_far(blocks):
    groups = [[r + 8 * k for k in range(8)] for r in range(8)]
    flat = blocks.reshape(-1, blocks.shape[2])
    return lax.all_gather(flat, "sp", axis=0, tiled=True, axis_index_groups=groups)


def layer_of(far, layer):
    parts = far.reshape(8, -1, ROWS, far.shape[1])
    return parts[:, layer].reshape(-1, far.shape[1])


def per_device(tokens, norm_gain, w_outer, w_inner, w_value, w_back, taps):
    count, width = tokens.shape
    feats = w_back.shape[2]
    rank = lax.axis_index("tp")
    tp = lax.axis_size("tp")
    layers = w_outer.shape[0]
    rows = count + HALO

    packed = pack(w_outer, w_inner, w_value, w_back)
    before = lax.ppermute(tokens[count - HALO :], "sp", [(i, i + 1) for i in range(63)])
    far = gather_far(packed)
    twos = []
    for layer in range(layers):
        twos.append(exchange(layer_of(far, layer), 2))
    partner = swap_cores(far)
    held = []
    for layer in range(layers):
        both = jnp.concatenate([layer_of(far, layer), layer_of(partner, layer)], axis=0)
        one = exchange(both, 1)
        near = jnp.concatenate([one, twos[layer]], axis=0)
        if layer == 0:
            resid = lax.dynamic_slice_in_dim(
                jnp.concatenate([before, tokens], axis=0), rank * feats, feats, 1
            )
            near, before, resid = lax.optimization_barrier((near, before, resid))
        held.append((both, near, swap_cores(near)))

    weights = pltpu.VMEM((width, 256), BF16)
    back_shape = jax.ShapeDtypeStruct((1024, 256), BF16)
    flops = 2 * rows * width * 256
    send = functools.partial(
        lax.all_to_all, axis_name="tp", split_axis=0, concat_axis=0, tiled=True
    )

    gated, back = call(
        first_kernel,
        [jax.ShapeDtypeStruct((tp, count // 2 + HALO, 128), BF16), back_shape],
        7, [weights], flops, 8 << 20,
    )(tokens, before, norm_gain, taps, *held[0])
    whole = send(gated)
    spread = pl.pallas_call(
        functools.partial(back_kernel, True),
        out_shape=jax.ShapeDtypeStruct((tp, rows, feats), BF16),
        in_specs=[VMEM] * 3,
        out_specs=pl.BlockSpec(memory_space=pltpu.HBM),
        scratch_shapes=[
            pltpu.VMEM((rows, feats), BF16),
            pltpu.SemaphoreType.DMA((tp,)),
        ],
        compiler_params=pltpu.CompilerParams(vmem_limit_bytes=62 << 20),
        cost_estimate=pl.CostEstimate(
            flops=2 * rows * 1024 * 256, bytes_accessed=4 << 20, transcendentals=0
        ),
    )(whole, back, resid)
    current = send(spread)
    gated, back, resid = call(
        second_kernel,
        [
            jax.ShapeDtypeStruct((tp, count // 2, 128), BF16),
            back_shape,
            jax.ShapeDtypeStruct((rows, feats), BF16),
        ],
        6, [weights], flops, 8 << 20,
    )(current, norm_gain, taps, *held[1])
    whole = send(gated)
    (result,) = call(
        functools.partial(back_kernel, False),
        [jax.ShapeDtypeStruct((count, feats), BF16)],
        3, [], 2 * rows * 1024 * 256, 4 << 20,
    )(whole, back, resid)
    return result


def solution(mesh):
    in_specs = (
        P("sp", None),
        P(),
        P(None, "sp", "tp"),
        P(None, "sp", "tp"),
        P(None, "sp", "tp"),
        P(None, "sp", "tp"),
        P(None, None, "tp"),
    )
    out_specs = P("sp", "tp")
    return jax.shard_map(
        per_device, mesh=mesh, in_specs=in_specs, out_specs=out_specs, check_vma=False
    )
```
